256 devices in a mesh: grp: 2 (over y), kv: 32 (over z, core), tp: 4 (over x).
Axes of the slice: x: 4, y: 2, z: 16, core: 2. Of those that a mesh axis runs over, the one named last changes fastest.
The devices are a block of a 4x16x16 slice.
Arguments:
- hidden: bfloat16 [2048, 4096], P('grp', 'kv'), parts along dimension 0, may hold values from -64 to 64
- norm_gain: bfloat16 [4096], replicated, may hold values from 0.099609375 to 1.8984375
- w_query: bfloat16 [4096, 2048], P('kv', 'tp'), may hold values from -0.09375 to 0.09375
- w_key: bfloat16 [4096, 2048], P('kv', 'tp'), may hold values from -0.09375 to 0.09375
- w_value: bfloat16 [4096, 2048], P('kv', 'tp'), may hold values from -0.09375 to 0.09375
- w_gate: bfloat16 [4096, 2048], P('kv', 'tp'), may hold values from -0.09375 to 0.09375
- w_decay: bfloat16 [4096, 16], P(None, 'tp'), may hold values from -0.09375 to 0.09375
- w_write: bfloat16 [4096, 16], P(None, 'tp'), may hold values from -0.09375 to 0.09375
- decay_rate: float32 [16], P('tp'), may hold values from 0.02 to 1
- head_gain: bfloat16 [128], replicated, may hold values from 0.099609375 to 1.8984375
- w_output: bfloat16 [2048, 4096], P('tp', 'kv'), may hold values from -0.125 to 0.125
- state: float32 [512, 16, 16384], P(('grp', 'kv'), 'tp'), parts along dimension 0, may hold values from -6 to 6
- prev_keys: bfloat16 [512, 4, 2048], P(('grp', 'kv'), None, 'tp'), parts along dimension 0, may hold values from -6 to 6
- prev_values: bfloat16 [512, 4, 2048], P(('grp', 'kv'), None, 'tp'), parts along dimension 0, may hold values from -6 to 6
- prev_decay: float32 [512, 4, 16], P(('grp', 'kv'), None, 'tp'), parts along dimension 0, may hold values from -1 to -0.02
- prev_write: float32 [512, 4, 16], P(('grp', 'kv'), None, 'tp'), parts along dimension 0, may hold values from 0.05 to 0.95
- accepted: int32 [512], P(('grp', 'kv')), parts along dimension 0, may hold values from 0 to 4
Outputs:
- mixed: bfloat16 [2048, 4096], P('grp', 'kv'), parts along dimension 0
- state_out: float32 [512, 16, 16384], P(('grp', 'kv'), 'tp'), parts along dimension 0
The draws below stay inside these ranges and needn't reach their ends.
There are 2 independent parts, one for each index of `grp`. The reference program is written for one: setup_inputs(seed, part) draws one part's arguments, and reference() takes and returns one part's arrays. A program takes and returns all parts, laid end to end along the dimension named above; an argument that names none is the same for every part. Nothing has to cross between parts.
All inputs are finite; a program needn't handle non-finite values.
Results may differ from the reference program's by a relative error of at most 0.0069.
Values may be sent and summed in bfloat16 or wider, within the bound.
A program may use at most 64 MiB of HBM per device.

```python
import math
import jax
import jax.numpy as jnp
from jax import lax

D = 4096
H = 16
DK = 128
PROP = 4
SEQS = 256
TOKENS = 1024
HID = 2048


def draw_hidden(key, part):
    key_rows, key_cols, key_base = jax.random.split(jax.random.fold_in(key, 11), 3)
    columns = jnp.arange(D, dtype=jnp.float32)
    column_scale = jnp.exp(math.log(3.0) * columns / D + jax.random.uniform(key_cols, (D,), jnp.float32, -0.35, 0.35))
    row_scale = jnp.exp(jax.random.uniform(key_rows, (TOKENS, 1), jnp.float32, 0.0, math.log(10.0)))
    base = jax.random.normal(key_base, (TOKENS, D), jnp.float32)
    base = jnp.clip(base, -5.0, 5.0)
    return jnp.clip(0.3 * base * row_scale * column_scale, -64.0, 64.0).astype(jnp.bfloat16)


def plant(drawn, own_key, low, high):
    spot = [jax.random.randint(jax.random.fold_in(own_key, axis), (), 0, length) for axis, length in enumerate(drawn.shape)]
    widest = drawn.shape.index(max(drawn.shape))
    beside = spot[:widest] + [(spot[widest] + 1) % drawn.shape[widest]] + spot[widest + 1:]
    return drawn.at[tuple(spot)].set(low).at[tuple(beside)].set(high)


def block_levels(own_key, extent, pieces, least, top_value):
    loudness = 1.0
    for axis_at, parts in pieces:
        steps = jax.random.uniform(jax.random.fold_in(jax.random.fold_in(own_key, 6), axis_at), (parts,), jnp.float32, least / len(pieces), top_value / len(pieces))
        loudness = loudness * jnp.repeat(jnp.exp(steps), extent[axis_at] // parts).reshape((-1,) + (1,) * (len(extent) - 1 - axis_at))
    return loudness


def normal_values(key, shape, spread, most, cuts=(), kind=jnp.bfloat16):
    values = spread * jax.random.normal(key, shape, jnp.float32)
    if cuts:
        values = values * block_levels(key, shape, cuts, -0.22, 0.18)
    return jnp.clip(values, -most, most).astype(kind)


def setup_inputs(seed: int = 0, part: int = 0) -> dict:
    arg_keys = jax.random.split(jax.random.key(seed), 18)
    part_splits = jax.random.split(jax.random.fold_in(arg_keys[17], part), 18)
    return {
        "hidden": draw_hidden(jax.random.fold_in(jax.random.fold_in(arg_keys[17], part), 71), part),
        "norm_gain": jnp.clip(1.0 + 0.18 * jax.random.normal(arg_keys[1], (D,), jnp.float32), 0.099609375, 1.8984375).astype(jnp.bfloat16),
        "w_query": normal_values(arg_keys[2], (D, HID), D ** -0.5, 0.09375, ((0, 32), (1, 4))),
        "w_key": normal_values(arg_keys[3], (D, HID), D ** -0.5, 0.09375, ((0, 32), (1, 4))),
        "w_value": normal_values(arg_keys[4], (D, HID), D ** -0.5, 0.09375, ((0, 32), (1, 4))),
        "w_gate": normal_values(arg_keys[5], (D, HID), D ** -0.5, 0.09375, ((0, 32), (1, 4))),
        "w_decay": normal_values(arg_keys[6], (D, H), D ** -0.5, 0.09375, ((1, 4),)),
        "w_write": normal_values(arg_keys[7], (D, H), D ** -0.5, 0.09375, ((1, 4),)),
        "decay_rate": jnp.clip(jnp.exp(math.log(1.0) - 3.912023 * jax.random.uniform(arg_keys[8], (H,), jnp.float32) ** block_levels(arg_keys[8], (H,), ((0, 4),), -0.2, 0.2)), 0.02, 1.0),
        "head_gain": jnp.clip(1.0 + 0.18 * jax.random.normal(arg_keys[9], (DK,), jnp.float32), 0.099609375, 1.8984375).astype(jnp.bfloat16),
        "w_output": normal_values(arg_keys[10], (HID, D), HID ** -0.5, 0.125, ((0, 4), (1, 32))),
        "state": normal_values(part_splits[11], (SEQS, H, DK * DK), 1.0, 6.0, ((0, 32), (1, 4)), jnp.float32),
        "prev_keys": normal_values(part_splits[12], (SEQS, PROP, HID), 1.0, 6.0, ((0, 32), (2, 4))),
        "prev_values": normal_values(part_splits[13], (SEQS, PROP, HID), 1.0, 6.0, ((0, 32), (2, 4))),
        "prev_decay": jnp.clip(-1.0 + 0.98 * jax.random.uniform(part_splits[14], (SEQS, PROP, H), jnp.float32) ** block_levels(part_splits[14], (SEQS, PROP, H), ((0, 32), (2, 4)), -0.2, 0.2), -1.0, -0.02),
        "prev_write": jnp.clip(0.05 + 0.9 * jax.random.uniform(part_splits[15], (SEQS, PROP, H), jnp.float32) ** block_levels(part_splits[15], (SEQS, PROP, H), ((0, 32), (2, 4)), -0.2, 0.2), 0.05, 0.95),
        "accepted": plant(jax.random.randint(part_splits[16], (SEQS,), 0, PROP + 1), jax.random.fold_in(part_splits[16], 1), 0, PROP).astype(jnp.int32),
    }


EPSILON = 1e-06

def unit_rows(values):
    return values * lax.rsqrt(lax.optimization_barrier(jnp.sum(values * values, axis=-1, keepdims=True)) + EPSILON)

def update_state(state_matrix, single_key_row, value_row, decay_row, write_row):
    state_matrix = state_matrix * jnp.exp(decay_row)[:, None, None]
    draft_token = jnp.einsum('xaf,xa->xf', state_matrix, single_key_row, precision=lax.Precision.HIGHEST)
    return state_matrix + write_row[:, None, None] * single_key_row[:, :, None] * (value_row - draft_token)[:, None, :]

def one_sequence(items):
    carried_state, query_rows, keys, values, log_decay, writes, old_keys, old_values, old_decay, old_writes = items
    for token_position in range(PROP):
        carried_state = update_state(carried_state, old_keys[token_position], old_values[token_position], old_decay[token_position], old_writes[token_position])
    taken_state = carried_state
    produced_output = []
    for token_position in range(PROP):
        carried_state = update_state(carried_state, keys[token_position], values[token_position], log_decay[token_position], writes[token_position])
        produced_output.append(jnp.einsum('xaf,xa->xf', carried_state, query_rows[token_position], precision=lax.Precision.HIGHEST))
    return (taken_state, jnp.stack(produced_output))

def reference(hidden, norm_gain, w_query, w_key, w_value, w_gate, w_decay, w_write, decay_rate, head_gain, w_output, state, prev_keys, prev_values, prev_decay, prev_write, accepted):
    wide = hidden.astype(jnp.float32)
    inverse = lax.rsqrt(lax.optimization_barrier(jnp.mean(wide * wide, axis=1)) + EPSILON)
    scaled = (wide * norm_gain.astype(jnp.float32)).astype(jnp.bfloat16)
    seqs = state.shape[0]

    def project(weight):
        return jnp.dot(scaled, weight, preferred_element_type=jnp.float32) * inverse[:, None]

    def split_heads(block):
        return block.reshape(seqs, PROP, H, DK)
    query_rows = unit_rows(split_heads(project(w_query))) * DK ** (-0.5)
    keys = unit_rows(split_heads(project(w_key)))
    values = split_heads(project(w_value))
    gates = split_heads(project(w_gate))
    log_decay = (-decay_rate * jax.nn.softplus(project(w_decay))).reshape(seqs, PROP, H)
    writes = jax.nn.sigmoid(project(w_write)).reshape(seqs, PROP, H)
    taken = jnp.arange(PROP, dtype=jnp.int32)[None, :] < accepted[:, None]
    old_keys = unit_rows(split_heads(prev_keys.astype(jnp.float32)))
    old_values = split_heads(prev_values.astype(jnp.float32))
    old_decay = jnp.where(taken[:, :, None], prev_decay, 0.0)
    old_writes = jnp.where(taken[:, :, None], prev_write, 0.0)
    carried_state = state.reshape(seqs, H, DK, DK)
    taken_states, outputs = lax.map(one_sequence, (carried_state, query_rows, keys, values, log_decay, writes, old_keys, old_values, old_decay, old_writes))
    normed = outputs * lax.rsqrt(lax.optimization_barrier(jnp.mean(outputs * outputs, axis=-1, keepdims=True)) + EPSILON)
    normed = normed * head_gain.astype(jnp.float32) * jax.nn.silu(gates)
    heads_out = normed.reshape(seqs * PROP, H * DK).astype(jnp.bfloat16)
    total = jnp.dot(heads_out, w_output, preferred_element_type=jnp.float32)
    return (total.astype(jnp.bfloat16), taken_states.reshape(seqs, H, DK * DK))
```

```python
import functools

import jax
import jax.numpy as jnp
from jax import lax
from jax.experimental import pallas as pl
from jax.experimental.pallas import tpu as pltpu
from jax.sharding import PartitionSpec as P

MESH = pl.DeviceIdType.MESH
GRP_KV = ("grp", "kv")
EPSILON = 1e-06
F32 = jnp.float32
BF16 = jnp.bfloat16
PIECES = 4
WIDE_HOPS = 1
RELAY = 2


def split(value):
    high = value.astype(BF16)
    return high, (value - high.astype(F32)).astype(BF16)


def dot(a, b, dims=((1,), (0,))):
    return lax.dot_general(a, b, (dims, ((), ())), preferred_element_type=F32)


def lane_sum(value):
    return jnp.sum(value, axis=-1, keepdims=True)


def body(
    sizes,
    hidden, gain, w_query, w_key, w_value, w_gate, w_decay, w_write, rate, head_gain, w_output,
    state, prev_keys, prev_values, old_scalars,
    mixed, state_out,
    raw, gains, scaled, held_w, sent_w, squares, weights_small, partial,
    out_bf, in_bf, out_wide, in_wide, out_small, in_small,
    sums, halves, small, small_t,
    s_old, s_high, s_low, s_new, old_k, old_v, reads, rows_k, rows_u,
    heads_f32, heads_bf, gathered, flat, w_out_all, result,
    load_sem, pair_send, pair_recv, ring_send, ring_recv, swap_send, swap_recv,
    w_send, w_recv, head_send, head_recv, relay_send, relay_recv, twin_send, twin_recv,
    mix_send, mix_recv, store_sem,
):
    zs, tps, seqs, props, heads, hs = sizes
    half = zs // 2
    kv = lax.axis_index("kv")
    tp = lax.axis_index("tp")
    z = kv // 2
    core = lax.rem(kv, 2)
    other = 1 - core
    twin = z * 2 + other
    width = heads * hs
    rows = scaled.shape[0] // zs
    mine = rows // 2
    feats = hidden.shape[1]
    part = held_w.shape[1] // PIECES
    model = gain.shape[0] * gain.shape[1]

    def at_z(step):
        return lax.rem(z + step + 2 * zs, zs)

    def kv_at(step):
        return at_z(step) * 2 + core

    def tp_at(step):
        return lax.rem(tp + step, tps)

    def remote(src, dst, send, recv, **where):
        return pltpu.make_async_remote_copy(
            src_ref=src, dst_ref=dst, send_sem=send, recv_sem=recv, device_id=where, device_id_type=MESH
        )

    loads = [
        pltpu.make_async_copy(hidden, raw.at[0], load_sem.at[0]),
        pltpu.make_async_copy(w_output, w_out_all.at[tp], load_sem.at[1]),
        pltpu.make_async_copy(state, s_old, load_sem.at[2]),
    ]
    for load in loads:
        load.start()

    def weight_loads(first, second):
        return [
            pltpu.make_async_copy(first[0], held_w.at[pl.ds(0, feats), pl.ds(0, width)], load_sem.at[3]),
            pltpu.make_async_copy(first[1], held_w.at[pl.ds(0, feats), pl.ds(width, width)], load_sem.at[4]),
            pltpu.make_async_copy(second[0], sent_w.at[:, pl.ds(0, width)], load_sem.at[5]),
            pltpu.make_async_copy(second[1], sent_w.at[:, pl.ds(width, width)], load_sem.at[6]),
        ]

    by_core = (
        weight_loads((w_query, w_key), (w_gate, w_value)),
        weight_loads((w_gate, w_value), (w_query, w_key)),
    )
    for k in range(2):
        @pl.when(core == k)
        def _():
            for load in by_core[k]:
                load.start()

    barrier = pltpu.get_barrier_semaphore()
    near = [twin] + [kv_at(d * h) for h in range(1, RELAY + 1) for d in (1, -1)]
    for peer in near:
        pl.semaphore_signal(barrier, inc=1, device_id={"kv": peer}, device_id_type=MESH)
    for step in range(1, tps):
        pl.semaphore_signal(barrier, inc=1, device_id={"tp": tp_at(step)}, device_id_type=MESH)

    gains[...] = gain[...].astype(F32)
    small[...] = jnp.zeros_like(small)
    at_own = pl.multiple_of(kv * feats, feats)
    at_twin = pl.multiple_of(twin * feats, feats)
    for k, small_weight in enumerate((w_decay, w_write)):
        @pl.when(core == k)
        def _():
            w = jnp.concatenate(
                [small_weight[:, pl.ds(at_own, feats)], small_weight[:, pl.ds(at_twin, feats)]], axis=1
            )
            weights_small[0:heads, :] = w.astype(F32)
    weights_small[heads:, :] = jnp.zeros((8 - heads, 2 * feats), F32)

    pl.semaphore_wait(barrier, len(near) + tps - 1)

    loads[0].wait()
    for load in by_core[0]:
        load.wait()
    pair = [
        remote(raw.at[0], raw.at[1], pair_send.at[0], pair_recv.at[0], kv=twin),
        remote(sent_w, held_w.at[pl.ds(feats, feats), :], pair_send.at[1], pair_recv.at[1], kv=twin),
    ]
    for copy in pair:
        copy.start()
    loads[1].wait()
    w_copies = []
    for step in range(1, tps):
        w_copies.append(
            remote(w_out_all.at[tp], w_out_all.at[tp], w_send.at[step - 1], w_recv.at[step - 1], tp=tp_at(step))
        )
        w_copies[-1].start()

    def scale(slot, who):
        wide = raw[slot].astype(F32)
        scaled[:, slot * feats:(slot + 1) * feats] = (wide * gains[pl.ds(who, 1), :]).astype(BF16)
        wide = wide * wide
        squares[0, :, slot * feats:(slot + 1) * feats], squares[1, :, slot * feats:(slot + 1) * feats] = split(wide)

    scale(0, kv)
    for copy in pair:
        copy.wait()
    scale(1, twin)

    w_small = weights_small[...].astype(BF16)
    ones_row = (lax.broadcasted_iota(jnp.int32, (8, 2 * feats), 0) == heads).astype(BF16)

    def chunk_dot(chunk, slot):
        at = pl.ds(pl.multiple_of(chunk * rows, rows), rows)
        partial[slot] = dot(scaled[at, :], held_w[...])

    def small_dot(chunk):
        at = pl.ds(pl.multiple_of(chunk * rows, rows), rows)
        over = ((1,), (1,))
        return (
            dot(w_small, scaled[at, :], over)
            + dot(ones_row, squares[0, at, :], over)
            + dot(ones_row, squares[1, at, :], over)
        )

    taken_reads = []
    old = {}

    def old_reads(seq):
        for h in range(heads):
            matrix = s_old[pl.ds(seq * hs * heads + h, hs, stride=heads), :]
            high, low = split(matrix)
            key_rows = old_k[h, seq * props:(seq + 1) * props, :]
            key_rows = jnp.concatenate([key_rows, jnp.zeros_like(key_rows)], axis=0).astype(BF16)
            reads[h, seq * 8:(seq + 1) * 8, :] = dot(key_rows, high) + dot(key_rows, low)

    def by_head(fn):
        return jnp.concatenate([fn(h) for h in range(heads)], axis=1)

    def load_rows(ref, at):
        return by_head(lambda h: ref[h, at, :])

    def store_rows(ref, at, value):
        for h in range(heads):
            ref[h, at, :] = head(value, h)

    def head(value, h):
        return value[:, h * hs:(h + 1) * hs]

    def spread(value):
        return by_head(lambda h: jnp.broadcast_to(value[:, h:h + 1], (seqs, hs)))

    def head_sums(value):
        return by_head(lambda h: jnp.broadcast_to(lane_sum(head(value, h)), (seqs, hs)))

    def unit(value):
        return value * lax.rsqrt(head_sums(value) + EPSILON)

    def unit_factor(value):
        return lax.rsqrt(head_sums(value) + EPSILON)

    def updates(keys, values, log_decay, writes, state_reads):
        totals, fresh = [], []
        for p in range(props):
            totals.append(log_decay[p] if p == 0 else totals[-1] + log_decay[p])
            value = values[p] - jnp.exp(totals[p]) * state_reads[p]
            for e in range(p):
                value = value - jnp.exp(totals[p] - totals[e]) * head_sums(keys[p] * keys[e]) * fresh[e]
            fresh.append(writes[p] * value)
        return totals, fresh

    def old_updates():
        keys, values, log_decay, writes, state_reads = [], [], [], [], []
        for p in range(props):
            key = load_rows(old_k, pl.ds(p, seqs, stride=props))
            factor = unit_factor(key * key)
            keys.append(key * factor)
            values.append(load_rows(old_v, pl.ds(p, seqs, stride=props)))
            log_decay.append(spread(old_scalars[:, p * heads:(p + 1) * heads]))
            writes.append(spread(old_scalars[:, (props + p) * heads:(props + p + 1) * heads]))
            state_reads.append(load_rows(reads, pl.ds(p, seqs, stride=8)) * factor)
        totals, fresh = updates(keys, values, log_decay, writes, state_reads)
        for p in range(props):
            store_rows(rows_k, pl.ds(p, seqs, stride=props), jnp.exp(totals[-1] - totals[p]) * keys[p])
            store_rows(rows_u, pl.ds(p, seqs, stride=props), fresh[p])
        old["decay"] = jnp.exp(totals[-1])

    def old_state(seq):
        for h in range(heads):
            at = pl.ds(seq * hs * heads + h, hs, stride=heads)
            k4 = rows_k[h, seq * props:(seq + 1) * props, :]
            u4 = rows_u[h, seq * props:(seq + 1) * props, :]
            k_high, u_high = k4.astype(BF16).astype(F32), u4.astype(BF16).astype(F32)
            lhs = jnp.concatenate([k_high, k4 - k_high, k_high, jnp.zeros_like(k4)], axis=0).astype(BF16)
            rhs = jnp.concatenate([u_high, u_high, u4 - u_high, jnp.zeros_like(u4)], axis=0).astype(BF16)
            matrix = s_old[at, :] * rows_u[h, seqs * props + seq:seqs * props + seq + 1, :] + dot(lhs, rhs, ((0,), (0,)))
            s_new[at, :] = matrix
            s_high[seq * heads + h], s_low[seq * heads + h] = split(matrix)

    stores = [
        pltpu.make_async_copy(
            s_new.at[pl.ds(s * hs * heads, hs * heads), :],
            state_out.at[pl.ds(s * hs * heads, hs * heads), :],
            store_sem.at[s],
        )
        for s in range(seqs)
    ]

    def side_work(step):
        if step == 1:
            loads[2].wait()
            for s in range(seqs):
                store_rows(old_k, pl.ds(s * props, props), prev_keys[s].astype(F32))
                store_rows(old_v, pl.ds(s * props, props), prev_values[s].astype(F32))
        if step in (1, 2):
            for s in range((step - 1) * seqs // 2, step * seqs // 2):
                old_reads(s)
        if step == 3:
            old_updates()
            store_rows(rows_u, pl.ds(seqs * props, seqs), old["decay"])
        if 4 <= step:
            per = seqs // (half - 4)
            for s in range((step - 4) * per, (step - 3) * per):
                old_state(s)
                stores[s].start()

    def is_wide(step, piece):
        return piece < PIECES // 2 and step >= half - WIDE_HOPS

    ring = {}

    def place(step, side, piece):
        if piece == PIECES:
            return out_small.at[step, side], in_small.at[step, side]
        if is_wide(step, piece):
            return (
                out_wide.at[step - half + WIDE_HOPS, side, piece],
                in_wide.at[step - half + WIDE_HOPS, side, piece],
            )
        return out_bf.at[step, side, piece], in_bf.at[step, side, piece]

    def first_step(side, piece):
        return 0 if piece % 2 == side else 1

    for step in range(half):
        chunk_dot(at_z(half - step), 0)
        if step > 0:
            chunk_dot(at_z(step - half), 1)
        small_part = [small_dot(at_z(half - step)), small_dot(at_z(step - half)) if step > 0 else None]
        side_work(step)
        for piece in range(PIECES + 1):
            for side in range(2):
                begins = first_step(side, piece)
                if step < begins:
                    continue
                if piece == PIECES:
                    value = small_part[side]
                else:
                    value = partial[side if step > 0 else 0, :, piece * part:(piece + 1) * part]
                if step > begins:
                    before = ring[step - 1, side, piece]
                    before.wait_recv()
                    value = value + place(step - 1, side, piece)[1][...].astype(F32)
                src, dst = place(step, side, piece)
                src[...] = value.astype(src.dtype)
                copy = remote(
                    src, dst,
                    ring_send.at[step, side, piece], ring_recv.at[step, side, piece],
                    kv=kv_at(1 - 2 * side),
                )
                copy.start()
                ring[step, side, piece] = copy
    chunk_dot(z, 0)
    own_small = small_dot(z)
    swaps = []
    for piece in range(PIECES + 1):
        value = own_small if piece == PIECES else partial[0, :, piece * part:(piece + 1) * part]
        for side in range(2):
            ring[half - 1, side, piece].wait_recv()
            value = value + place(half - 1, side, piece)[1][...].astype(F32)
        if piece == PIECES:
            small[core, :, 0:rows] = value
        else:
            blocks = pl.ds(piece * (part // hs), part // hs)
            for n in range(part // hs):
                for owner in range(2):
                    sums[owner, piece * (part // hs) + n] = value[owner * mine:(owner + 1) * mine, n * hs:(n + 1) * hs]
            swap = remote(
                sums.at[other, blocks], halves.at[core, blocks], swap_send.at[piece], swap_recv.at[piece], kv=twin
            )
            swap.start()
            swaps.append(swap)
    swap = remote(small.at[core], small.at[core], swap_send.at[PIECES], swap_recv.at[PIECES], kv=twin)
    swap.start()
    swaps.append(swap)
    halves[core] = sums[core]
    for swap in swaps:
        swap.wait()

    for k in range(2):
        small_t[k, :, 0:8] = jnp.transpose(small[k])

    def piece_of(kind, at):
        return by_head(lambda h: halves[kind // 2, (kind % 2) * heads + h, at, :])

    for s in range(seqs):
        at = pl.ds(s * props, props)
        q4, k4 = piece_of(0, at), piece_of(1, at)
        for h in range(heads):
            cols = slice(h * hs, (h + 1) * hs)
            lhs = jnp.concatenate([q4[:, cols], k4[:, cols]], axis=0)
            high = lhs.astype(BF16).astype(F32)
            both = jnp.concatenate([high, lhs - high], axis=0).astype(BF16)
            first = dot(both, s_high[s * heads + h])
            second = dot(high.astype(BF16), s_low[s * heads + h])
            reads[h, s * 8:(s + 1) * 8, :] = first[:8] + first[8:] + second

    queries, keys, values, log_decay, writes, reads_q, reads_k, gates = ([] for _ in range(8))
    rates = jnp.broadcast_to(rate[...], (seqs, heads))
    for p in range(props):
        at = pl.ds(p, seqs, stride=props)
        at_small = pl.ds(core * mine + p, seqs, stride=props)
        cols_d, cols_w = small_t[0, at_small, :], small_t[1, at_small, :]
        inverse = lax.rsqrt(cols_d[:, heads:heads + 1] * (1.0 / model) + EPSILON)
        pre_decay = cols_d[:, 0:heads] * inverse
        pre_write = cols_w[:, 0:heads] * inverse
        soft = jnp.maximum(pre_decay, 0.0) + jnp.log1p(jnp.exp(-jnp.abs(pre_decay)))
        log_decay.append(spread(-rates * soft))
        writes.append(spread(1.0 / (1.0 + jnp.exp(-pre_write))))
        q, k = piece_of(0, at) * inverse, piece_of(1, at) * inverse
        q_factor = unit_factor(q * q) * hs ** (-0.5)
        k_factor = unit_factor(k * k)
        queries.append(q * q_factor)
        keys.append(k * k_factor)
        gates.append(piece_of(2, at) * inverse)
        values.append(piece_of(3, at) * inverse)
        reads_q.append(load_rows(reads, pl.ds(p, seqs, stride=8)) * (q_factor * inverse))
        reads_k.append(load_rows(reads, pl.ds(props + p, seqs, stride=8)) * (k_factor * inverse))
    totals, fresh = updates(keys, values, log_decay, writes, reads_k)
    head_scale = by_head(lambda h: jnp.broadcast_to(head_gain[...].astype(F32), (seqs, hs)))
    for p in range(props):
        out = jnp.exp(totals[p]) * reads_q[p]
        for e in range(p + 1):
            out = out + jnp.exp(totals[p] - totals[e]) * head_sums(queries[p] * keys[e]) * fresh[e]
        out = out * lax.rsqrt(head_sums(out * out) * (1.0 / hs) + EPSILON)
        gate = gates[p]
        out = out * head_scale * (gate / (1.0 + jnp.exp(-gate)))
        store_rows(heads_f32, pl.ds(p, seqs, stride=props), out)

    per_tp = mine // tps
    for t in range(tps):
        heads_bf[t] = load_rows(heads_f32, pl.ds(t * per_tp, per_tp)).astype(BF16)
    head_copies = []
    for step in range(1, tps):
        copy = remote(
            heads_bf.at[tp_at(step)], gathered.at[kv, tp], head_send.at[step - 1], head_recv.at[step - 1],
            tp=tp_at(step),
        )
        copy.start()
        head_copies.append(copy)
    gathered[kv, tp] = heads_bf[tp]
    for copy in head_copies:
        copy.wait_recv()

    relays = {}
    twins = []

    def to_twin(who, n):
        copy = remote(gathered.at[who], gathered.at[who], twin_send.at[n], twin_recv.at[n], kv=twin)
        copy.start()
        twins.append(copy)

    reach = (half, zs - 1 - half)
    ahead = lax.rem(1 - 2 * core + zs, zs)
    for hop in range(0, half, RELAY):
        for side in range(2):
            if hop >= reach[side] or (hop == 0 and side == 1 and False):
                continue
            sign = 1 - 2 * side
            from_kv = lax.rem(z + (zs - hop) * sign * (1 - 2 * core) + 2 * zs * zs, zs) * 2 + core
            if hop > 0:
                relays[side, hop].wait_recv()
            for far in range(RELAY, 0, -1):
                if hop + far > reach[side]:
                    continue
                to = lax.rem(z + sign * (1 - 2 * core) * far + zs, zs) * 2 + core
                copy = remote(
                    gathered.at[from_kv], gathered.at[from_kv],
                    relay_send.at[side, hop + far - 1], relay_recv.at[side, hop + far - 1], kv=to,
                )
                copy.start()
                relays[side, hop + far] = copy
        if hop == 0:
            to_twin(kv, 0)
        for side in range(2):
            sign = 1 - 2 * side
            for far in range(1, RELAY + 1) if hop > 0 else ():
                at_hop = hop - RELAY + far
                if at_hop > reach[side]:
                    continue
                if at_hop % RELAY or at_hop + RELAY > half or at_hop >= reach[side]:
                    relays[side, at_hop].wait_recv()
                who = lax.rem(z - at_hop * sign * (1 - 2 * core) + 2 * zs, zs) * 2 + core
                to_twin(who, len(twins))
    for side in range(2):
        sign = 1 - 2 * side
        for at_hop in range(half - RELAY + 1, reach[side] + 1):
            relays[side, at_hop].wait_recv()
            who = lax.rem(z - at_hop * sign * (1 - 2 * core) + 2 * zs, zs) * 2 + core
            to_twin(who, len(twins))
    for copy in twins:
        copy.wait_recv()
    for copy in w_copies:
        copy.wait_recv()

    for c in range(zs):
        for t in range(tps):
            both = jnp.concatenate(
                [gathered[2 * c, t].astype(F32), gathered[2 * c + 1, t].astype(F32)], axis=0
            )
            flat[c * 2 * per_tp:(c + 1) * 2 * per_tp, t * width:(t + 1) * width] = both.astype(BF16)
    total = dot(flat[:, 0:width], w_out_all[0])
    for t in range(1, tps):
        total = total + dot(flat[:, t * width:(t + 1) * width], w_out_all[t])
    result[...] = total.reshape(result.shape).astype(BF16)
    mix_copies = []
    for step in range(1, tps):
        copy = remote(result, mixed.at[:, tp], mix_send.at[step - 1], mix_recv.at[step - 1], tp=tp_at(step))
        copy.start()
        mix_copies.append(copy)
    own = pltpu.make_async_copy(result, mixed.at[:, tp], store_sem.at[seqs])
    own.start()

    for copy in ring.values():
        copy.wait_send()
    for copy in w_copies + head_copies + list(relays.values()) + twins:
        copy.wait_send()
    for copy in stores:
        copy.wait()
    own.wait()
    for copy in mix_copies:
        copy.wait()


def per_device(
    sizes,
    hidden, norm_gain, w_query, w_key, w_value, w_gate, w_decay, w_write, decay_rate, head_gain, w_output,
    state, prev_keys, prev_values, prev_decay, prev_write, accepted,
):
    zs, tps = sizes
    tokens, feats = hidden.shape
    heads, width = w_decay.shape[1], w_query.shape[1]
    hs = width // heads
    seqs, props = prev_keys.shape[:2]
    rows = tokens // zs
    half = zs // 2
    part = 2 * width // PIECES
    per_tp = seqs * props // tps
    taken = (jnp.arange(props, dtype=jnp.int32)[None, :] < accepted[:, None])[..., None]
    old_scalars = jnp.concatenate(
        [jnp.where(taken, prev_decay, 0.0).reshape(seqs, -1), jnp.where(taken, prev_write, 0.0).reshape(seqs, -1)],
        axis=1,
    )
    lines = state.reshape(seqs, heads, hs, hs).transpose(0, 2, 1, 3).reshape(seqs * heads * hs, hs)
    any_ = pl.BlockSpec(memory_space=pl.ANY)
    vmem = pl.BlockSpec(memory_space=pltpu.VMEM)
    dma = pltpu.SemaphoreType.DMA
    scratch = [
        pltpu.VMEM((2, tokens, feats), BF16),
        pltpu.VMEM((norm_gain.shape[0] // feats, feats), F32),
        pltpu.VMEM((tokens, 2 * feats), BF16),
        pltpu.VMEM((2 * feats, 2 * width), BF16),
        pltpu.VMEM((feats, 2 * width), BF16),
        pltpu.VMEM((2, tokens, 2 * feats), BF16),
        pltpu.VMEM((8, 2 * feats), F32),
        pltpu.VMEM((2, rows, 2 * width), F32),
        pltpu.VMEM((half, 2, PIECES, rows, part), BF16),
        pltpu.VMEM((half, 2, PIECES, rows, part), BF16),
        pltpu.VMEM((max(WIDE_HOPS, 1), 2, PIECES // 2, rows, part), F32),
        pltpu.VMEM((max(WIDE_HOPS, 1), 2, PIECES // 2, rows, part), F32),
        pltpu.VMEM((half, 2, 8, rows), F32),
        pltpu.VMEM((half, 2, 8, rows), F32),
        pltpu.VMEM((2, 2 * heads, rows // 2, hs), F32),
        pltpu.VMEM((2, 2 * heads, rows // 2, hs), F32),
        pltpu.VMEM((2, 8, 128), F32),
        pltpu.VMEM((2, 128, 128), F32),
        pltpu.VMEM(lines.shape, F32),
        pltpu.VMEM((seqs * heads, hs, hs), BF16),
        pltpu.VMEM((seqs * heads, hs, hs), BF16),
        pltpu.VMEM(lines.shape, F32),
        pltpu.VMEM((heads, seqs * props, hs), F32),
        pltpu.VMEM((heads, seqs * props, hs), F32),
        pltpu.VMEM((heads, seqs * 8, hs), F32),
        pltpu.VMEM((heads, seqs * props, hs), F32),
        pltpu.VMEM((heads, seqs * props + seqs, hs), F32),
        pltpu.VMEM((heads, seqs * props, hs), F32),
        pltpu.VMEM((tps, per_tp, width), BF16),
        pltpu.VMEM((2 * zs, tps, per_tp, width), BF16),
        pltpu.VMEM((2 * zs * per_tp, tps * width), BF16),
        pltpu.VMEM((tps,) + w_output.shape, BF16),
        pltpu.VMEM((2 * zs, per_tp, w_output.shape[1]), BF16),
        dma((7,)), dma((2,)), dma((2,)),
        dma((half, 2, PIECES + 1)), dma((half, 2, PIECES + 1)),
        dma((PIECES + 1,)), dma((PIECES + 1,)),
        dma((tps - 1,)), dma((tps - 1,)),
        dma((tps - 1,)), dma((tps - 1,)),
        dma((2, half)), dma((2, half)),
        dma((zs,)), dma((zs,)),
        dma((tps - 1,)), dma((tps - 1,)),
        dma((seqs + 1,)),
    ]
    mixed, new_lines = pl.pallas_call(
        functools.partial(body, (zs, tps, seqs, props, heads, hs)),
        out_shape=(
            jax.ShapeDtypeStruct((2 * zs, tps, per_tp, w_output.shape[1]), BF16),
            jax.ShapeDtypeStruct(lines.shape, F32),
        ),
        in_specs=[any_, vmem, any_, any_, any_, any_, vmem, vmem, vmem, vmem, any_, any_, vmem, vmem, vmem],
        out_specs=(any_, any_),
        scratch_shapes=scratch,
        compiler_params=pltpu.CompilerParams(
            collective_id=0, has_side_effects=True, vmem_limit_bytes=40 * 1024 * 1024
        ),
    )(
        hidden, norm_gain.reshape(-1, feats), w_query, w_key, w_value, w_gate, w_decay.T, w_write.T,
        decay_rate.reshape(1, heads), head_gain.reshape(1, hs), w_output, lines, prev_keys, prev_values, old_scalars,
    )
    mixed = mixed.reshape(tokens, w_output.shape[1])
    new_state = new_lines.reshape(seqs, hs, heads, hs).transpose(0, 2, 1, 3).reshape(state.shape)
    return mixed, new_state


def solution(mesh):
    sizes = (mesh.shape["kv"] // 2, mesh.shape["tp"])
    in_specs = (
        P("grp", "kv"),
        P(),
        P("kv", "tp"),
        P("kv", "tp"),
        P("kv", "tp"),
        P("kv", "tp"),
        P(None, "tp"),
        P(None, "tp"),
        P("tp"),
        P(),
        P("tp", "kv"),
        P(GRP_KV, "tp", None),
        P(GRP_KV, None, "tp"),
        P(GRP_KV, None, "tp"),
        P(GRP_KV, None, "tp"),
        P(GRP_KV, None, "tp"),
        P(GRP_KV),
    )
    out_specs = (P("grp", "kv"), P(GRP_KV, "tp", None))
    return jax.shard_map(
        functools.partial(per_device, sizes), mesh=mesh, in_specs=in_specs, out_specs=out_specs, check_vma=False
    )
```
